32 devices in a mesh: sp: 4 (over y, core), dp: 8 (over z, x).
Axes of the slice: x: 2, y: 2, z: 4, core: 2. Of those that a mesh axis runs over, the one named last changes fastest.
Arguments:
- query_rows: bfloat16 [8, 512, 4, 128], P('dp', 'sp'), may hold values from -6 to 6
- key_rows: bfloat16 [8, 512, 4, 128], P('dp', 'sp'), may hold values from -6 to 6
- value_rows: bfloat16 [8, 512, 4, 128], P('dp', 'sp'), may hold values from -6 to 6
- map_weight: float32 [4], P('sp'), may hold values from 0.3 to 0.8
- head_gain: float32 [128], replicated, may hold values from 0.1 to 1.9
Outputs:
- mixed: bfloat16 [8, 512, 4, 128], P('dp', 'sp')
The draws below stay inside these ranges and needn't reach their ends.
All inputs are finite; a program needn't handle non-finite values.
Results may differ from the reference program's by a relative error of at most 0.0049.
Values may be sent and summed in bfloat16 or wider, within the bound.
A program may use at most 64 MiB of HBM per device.

```python
import math
import jax
import jax.numpy as jnp
from jax import lax

QK = 64
VD = 128
SEGMENT = 64
HEADS = 4
SEQ_LEN = 512
SEQS = 8


def drawn_pair(key):
    shape = (SEQS, SEQ_LEN, HEADS, 2 * QK)
    query_draw = 1.3 * jax.random.truncated_normal(jax.random.fold_in(key, 11), -4.5, 4.5, shape, jnp.float32)
    key_draw = 1.3 * jax.random.truncated_normal(jax.random.fold_in(key, 12), -4.5, 4.5, shape, jnp.float32)
    return (query_draw, key_draw)


def draw_query_rows(key, part):
    return drawn_pair(key)[0].astype(jnp.bfloat16)


def draw_key_rows(key, part):
    return drawn_pair(key)[1].astype(jnp.bfloat16)


def block_scale(key, extent, shards, low, top_value):
    def one(dim, blocks):
        steps = jax.random.uniform(jax.random.fold_in(jax.random.fold_in(key, 6), dim), (blocks,), jnp.float32, low / len(shards), top_value / len(shards))
        return jnp.repeat(jnp.exp(steps), extent[dim] // blocks).reshape((-1,) + (1,) * (len(extent) - dim - 1))

    loudness = one(*shards[0])
    for cut in shards[1:]:
        loudness = loudness * one(*cut)
    return loudness


def gaussian(rng, shape, deviation, limit, cuts=(), kind=jnp.bfloat16):
    drawn = deviation * jax.random.normal(rng, shape, jnp.float32)
    if cuts:
        drawn = drawn * block_scale(rng, shape, cuts, -0.22, 0.18)
    return jnp.clip(drawn, -limit, limit).astype(kind)


def setup_inputs(seed: int = 0) -> dict:
    seeds = jax.random.split(jax.random.key(seed), 6)
    query_rows = draw_query_rows(jax.random.fold_in(seeds[5], 71), 0)
    key_rows = draw_key_rows(jax.random.fold_in(seeds[5], 71), 0)
    value_rows = gaussian(seeds[2], (SEQS, SEQ_LEN, HEADS, VD), 1.0, 6.0, ((0, 8), (1, 4)))
    map_weight = jnp.clip(0.3 + 0.5 * jax.random.uniform(seeds[3], (HEADS,), jnp.float32) ** block_scale(seeds[3], (HEADS,), ((0, 4),), -0.2, 0.2), 0.3, 0.8)
    head_gain = jnp.clip(1.0 + 0.18 * jax.random.normal(seeds[4], (VD,), jnp.float32), 0.1, 1.9)
    return dict(query_rows=query_rows, key_rows=key_rows, value_rows=value_rows, map_weight=map_weight, head_gain=head_gain)


def attend_head(query_head, key_head, value_head, weight_two, head_gain):
    length = key_head.shape[0]
    block_len = math.gcd(length, 512)
    key_segment = jnp.arange(length, dtype=jnp.int32) // SEGMENT

    def one_block(start):
        query_block = lax.dynamic_slice_in_dim(query_head, start, block_len, 0)
        query_segment = (start + jnp.arange(block_len, dtype=jnp.int32)) // SEGMENT
        visible = key_segment[None, :] <= query_segment[:, None]
        parts = []
        for which in range(2):
            query_map = query_block[:, which * QK:(which + 1) * QK]
            key_map = key_head[:, which * QK:(which + 1) * QK]
            scores = jnp.dot(query_map, key_map.T, preferred_element_type=jnp.float32) * QK ** (-0.5)
            scores = jnp.where(visible, scores, -jnp.inf)
            scores = scores - lax.optimization_barrier(jnp.max(scores, axis=-1, keepdims=True))
            raised = jnp.exp(scores)
            weights = raised / lax.optimization_barrier(jnp.sum(raised, axis=-1, keepdims=True))
            parts.append(jnp.dot(weights.astype(jnp.bfloat16), value_head, preferred_element_type=jnp.float32))
        attended = parts[0] - weight_two * parts[1]
        mean_square = lax.optimization_barrier(jnp.mean(attended * attended, axis=-1, keepdims=True))
        return (attended * lax.rsqrt(mean_square + 1e-06) * head_gain).astype(jnp.bfloat16)
    starts = jnp.arange(length // block_len, dtype=jnp.int32) * block_len
    return lax.map(one_block, starts).reshape(length, value_head.shape[1])

def reference(query_rows, key_rows, value_rows, map_weight, head_gain):

    def per_sequence(items):
        query_seq, key_seq, value_seq = items
        result = lax.map(lambda group: attend_head(group[0], group[1], group[2], group[3], head_gain), (query_seq.transpose(1, 0, 2), key_seq.transpose(1, 0, 2), value_seq.transpose(1, 0, 2), map_weight))
        return result.transpose(1, 0, 2)
    return lax.map(per_sequence, (query_rows, key_rows, value_rows))
```

```python
import functools

import jax
import jax.numpy as jnp
from jax import lax
from jax.experimental import pallas as pl
from jax.experimental.pallas import tpu as pltpu
from jax.sharding import PartitionSpec as P

SEGMENT = 64
CORES = 2
UNROLL = 4
F32 = jnp.float32
BF16 = jnp.bfloat16


def order_matrix(rows, heads, tokens, back):
    out = lax.broadcasted_iota(jnp.int32, (rows, rows), 0)
    src = lax.broadcasted_iota(jnp.int32, (rows, rows), 1)
    if back:
        out, src = src, out
    wanted = (out % tokens) * heads + out // tokens
    return jnp.where(src == wanted, 1.0, 0.0).astype(BF16)


def kernel(
    n, heads, local, qk, hw_ref, gain_ref, q_hbm, k_hbm, v_hbm, out_ref,
    rows_in, staged, gq, gk, gv, made, back, in_sem, send_sem, recv_sem, osend_sem, orecv_sem,
):
    dim = q_hbm.shape[-1]
    mine = heads // n
    me = lax.axis_index("sp")
    tokens = max(16, 256 // heads)
    chunk = tokens * heads

    def there(p):
        return {"sp": p}

    sources = (k_hbm, v_hbm, q_hbm)
    loads = [pltpu.make_async_copy(sources[t], rows_in.at[t], in_sem.at[t]) for t in range(3)]
    for load in loads:
        load.start()
    barrier = pltpu.get_barrier_semaphore()
    for d in range(1, n):
        pl.semaphore_signal(
            barrier, inc=1, device_id=there(lax.rem(me + d, n)),
            device_id_type=pl.DeviceIdType.MESH,
        )
    order = order_matrix(chunk, heads, tokens, False)
    gathered = (gk, gv, gq)
    for t in range(3):
        loads[t].wait()
        for c in range(local // tokens):
            moved = jnp.dot(
                order, rows_in[t, c * chunk:(c + 1) * chunk], preferred_element_type=F32
            ).astype(BF16)
            for h in range(heads):
                staged[t, h, c * tokens:(c + 1) * tokens] = moved[h * tokens:(h + 1) * tokens]
    for t in range(3):
        for g in range(mine):
            gathered[t][g, pl.ds(pl.multiple_of(me * local, local), local)] = staged[t, me * mine + g]
    pl.semaphore_wait(barrier, n - 1)

    here = pl.ds(pl.multiple_of(me * local, local), local)

    def push(t, p):
        return pltpu.make_async_remote_copy(
            src_ref=staged.at[t, pl.ds(p * mine, mine)],
            dst_ref=gathered[t].at[:, here],
            send_sem=send_sem.at[t, p],
            recv_sem=recv_sem.at[t, me],
            device_id=there(p),
            device_id_type=pl.DeviceIdType.MESH,
        )

    base = (me // CORES) * CORES
    peers = [base + lax.rem(me - base + d, CORES) for d in range(1, CORES)]
    peers += [lax.rem(base + d, n) for d in range(CORES, n)]
    for p in peers:
        for t in range(3):
            push(t, p).start()

    def arrive(j):
        @pl.when(me != j)
        def _():
            for t in range(3):
                pltpu.make_async_remote_copy(
                    src_ref=staged.at[t, pl.ds(0, mine)],
                    dst_ref=gathered[t].at[:, pl.ds(pl.multiple_of(j * local, local), local)],
                    send_sem=send_sem.at[t, j],
                    recv_sem=recv_sem.at[t, j],
                    device_id=there(j),
                    device_id_type=pl.DeviceIdType.MESH,
                ).wait_recv()

    def give(i):
        return pltpu.make_async_remote_copy(
            src_ref=made.at[i],
            dst_ref=back.at[pl.ds(me * mine, mine)],
            send_sem=osend_sem.at[i],
            recv_sem=orecv_sem.at[me],
            device_id=there(i),
            device_id_type=pl.DeviceIdType.MESH,
        )

    lower = lax.broadcasted_iota(jnp.int32, (local, dim), 1) < qk
    gain = gain_ref[...]

    def attend(i, width, g):
        start = i * local if isinstance(i, int) else pl.multiple_of(i * local, local)
        query = gq[g, pl.ds(start, local)] * BF16(qk ** -0.5)
        zero = jnp.zeros_like(query)
        both = jnp.concatenate([jnp.where(lower, query, zero), jnp.where(lower, zero, query)], 0)
        scores = lax.dot_general(
            both, gk[g, :width], (((1,), (1,)), ((), ())), preferred_element_type=F32
        )
        row = lax.rem(lax.broadcasted_iota(jnp.int32, scores.shape, 0), local)
        col = lax.broadcasted_iota(jnp.int32, scores.shape, 1)
        visible = col // SEGMENT <= (start + row) // SEGMENT
        scores = jnp.where(visible, scores, -jnp.inf)
        raised = jnp.exp(scores - jnp.max(scores, axis=-1, keepdims=True))
        total = jnp.sum(raised, axis=-1, keepdims=True)
        part = jnp.dot(raised.astype(BF16), gv[g, :width], preferred_element_type=F32)
        part = part / total
        attended = part[:local] - hw_ref[g] * part[local:]
        square = jnp.mean(attended * attended, axis=-1, keepdims=True)
        made[i, g] = (attended * lax.rsqrt(square + 1e-06) * gain).astype(BF16)

    def finish(i):
        @pl.when(me != i)
        def _():
            give(i).start()

        @pl.when(me == i)
        def _():
            for g in range(mine):
                back[me * mine + g] = made[i, g]

    if n <= UNROLL:
        for i in range(n):
            arrive(i)
            for g in range(mine):
                attend(i, (i + 1) * local, g)
            finish(i)
    else:
        for j in range(n):
            arrive(j)

        def body(i, carry):
            for g in range(mine):
                attend(i, n * local, g)
            finish(i)
            return carry

        lax.fori_loop(0, n, body, 0)

    for p in peers:
        pltpu.make_async_remote_copy(
            src_ref=made.at[p],
            dst_ref=back.at[pl.ds(p * mine, mine)],
            send_sem=osend_sem.at[p],
            recv_sem=orecv_sem.at[p],
            device_id=there(p),
            device_id_type=pl.DeviceIdType.MESH,
        ).wait_recv()
    order = order_matrix(chunk, heads, tokens, True)
    for c in range(local // tokens):
        piece = jnp.concatenate(
            [back[h, c * tokens:(c + 1) * tokens] for h in range(heads)], 0
        )
        out_ref[c * chunk:(c + 1) * chunk] = jnp.dot(
            order, piece, preferred_element_type=F32
        ).astype(BF16)
    for p in peers:
        for t in range(3):
            push(t, p).wait_send()
        give(p).wait_send()


def on_device(n, query_rows, key_rows, value_rows, map_weight, head_gain):
    _, local, heads, dim = query_rows.shape
    mine = heads // n
    flat = (local * heads, dim)
    whole = n * local
    out = pl.pallas_call(
        functools.partial(kernel, n, heads, local, dim // 2),
        out_shape=jax.ShapeDtypeStruct(flat, BF16),
        in_specs=[
            pl.BlockSpec(memory_space=pltpu.SMEM),
            pl.BlockSpec(memory_space=pltpu.VMEM),
            pl.BlockSpec(memory_space=pl.ANY),
            pl.BlockSpec(memory_space=pl.ANY),
            pl.BlockSpec(memory_space=pl.ANY),
        ],
        out_specs=pl.BlockSpec(memory_space=pltpu.VMEM),
        scratch_shapes=[
            pltpu.VMEM((3,) + flat, BF16),
            pltpu.VMEM((3, heads, local, dim), BF16),
            pltpu.VMEM((mine, whole, dim), BF16),
            pltpu.VMEM((mine, whole, dim), BF16),
            pltpu.VMEM((mine, whole, dim), BF16),
            pltpu.VMEM((n, mine, local, dim), BF16),
            pltpu.VMEM((heads, local, dim), BF16),
            pltpu.SemaphoreType.DMA((3,)),
            pltpu.SemaphoreType.DMA((3, n)),
            pltpu.SemaphoreType.DMA((3, n)),
            pltpu.SemaphoreType.DMA((n,)),
            pltpu.SemaphoreType.DMA((n,)),
        ],
        compiler_params=pltpu.CompilerParams(collective_id=0, has_side_effects=True),
    )(
        map_weight,
        head_gain.reshape(1, dim),
        query_rows.reshape(flat),
        key_rows.reshape(flat),
        value_rows.reshape(flat),
    )
    return out.reshape(query_rows.shape)


def solution(mesh):
    rows = P("dp", "sp", None, None)
    return jax.shard_map(
        functools.partial(on_device, mesh.shape["sp"]),
        mesh=mesh,
        in_specs=(rows, rows, rows, P("sp"), P()),
        out_specs=rows,
        check_vma=False,
    )
```

```python
import functools

import jax
import jax.numpy as jnp
from jax import lax
from jax.experimental import pallas as pl
from jax.experimental.pallas import tpu as pltpu
from jax.sharding import PartitionSpec as P

SEGMENT = 64
CORES = 2
UNROLL = 4
KERNEL_BYTES = 32 * 1024 * 1024
F32 = jnp.float32
BF16 = jnp.bfloat16


def order_matrix(rows, heads, tokens, back):
    out = lax.broadcasted_iota(jnp.int32, (rows, rows), 0)
    src = lax.broadcasted_iota(jnp.int32, (rows, rows), 1)
    if back:
        out, src = src, out
    wanted = (out % tokens) * heads + out // tokens
    return jnp.where(src == wanted, 1.0, 0.0).astype(BF16)


def kernel(
    n, heads, local, qk, hw_ref, gain_hbm, q_hbm, k_hbm, v_hbm, back,
    rows_in, staged, gq, gk, gv, made, gain_ref, in_sem, send_sem, recv_sem, osend_sem, orecv_sem,
):
    dim = q_hbm.shape[-1]
    mine = heads // n
    me = lax.axis_index("sp")
    tokens = max(16, 256 // heads)
    chunk = tokens * heads

    def there(p):
        return {"sp": p}

    sources = (k_hbm, v_hbm, q_hbm)
    loads = [pltpu.make_async_copy(sources[t], rows_in.at[t], in_sem.at[t]) for t in range(3)]
    loads.append(pltpu.make_async_copy(gain_hbm, gain_ref, in_sem.at[3]))
    for load in loads:
        load.start()
    barrier = pltpu.get_barrier_semaphore()
    for d in range(1, n):
        pl.semaphore_signal(
            barrier, inc=1, device_id=there(lax.rem(me + d, n)),
            device_id_type=pl.DeviceIdType.MESH,
        )
    order = order_matrix(chunk, heads, tokens, False)
    gathered = (gk, gv, gq)
    here = pl.ds(pl.multiple_of(me * local, local), local)

    def push(t, p):
        return pltpu.make_async_remote_copy(
            src_ref=staged.at[t, pl.ds(p * mine, mine)],
            dst_ref=gathered[t].at[:, here],
            send_sem=send_sem.at[t, p],
            recv_sem=recv_sem.at[t, me],
            device_id=there(p),
            device_id_type=pl.DeviceIdType.MESH,
        )

    base = (me // CORES) * CORES
    peers = [lax.rem(base + d, n) for d in range(CORES, n)]
    peers += [base + lax.rem(me - base + d, CORES) for d in range(1, CORES)]
    for t in range(3):
        loads[t].wait()
        for c in range(local // tokens):
            moved = jnp.dot(
                order, rows_in[t, c * chunk:(c + 1) * chunk], preferred_element_type=F32
            ).astype(BF16)
            for h in range(heads):
                staged[t, h, c * tokens:(c + 1) * tokens] = moved[h * tokens:(h + 1) * tokens]
        if t == 0:
            pl.semaphore_wait(barrier, n - 1)
        push(t, peers[0]).start()
        for p in peers[n - CORES:]:
            push(t, p).start()
    for p in peers[1:n - CORES]:
        for t in range(3):
            push(t, p).start()
    for t in range(3):
        for g in range(mine):
            gathered[t][g, here] = staged[t, me * mine + g]

    def arrive(j):
        @pl.when(me != j)
        def _():
            for t in range(3):
                pltpu.make_async_remote_copy(
                    src_ref=staged.at[t, pl.ds(0, mine)],
                    dst_ref=gathered[t].at[:, pl.ds(pl.multiple_of(j * local, local), local)],
                    send_sem=send_sem.at[t, j],
                    recv_sem=recv_sem.at[t, j],
                    device_id=there(j),
                    device_id_type=pl.DeviceIdType.MESH,
                ).wait_recv()

    def give(i):
        return pltpu.make_async_remote_copy(
            src_ref=made.at[i],
            dst_ref=back.at[pl.ds(me * mine, mine)],
            send_sem=osend_sem.at[i],
            recv_sem=orecv_sem.at[me],
            device_id=there(i),
            device_id_type=pl.DeviceIdType.MESH,
        )

    lower = lax.broadcasted_iota(jnp.int32, (local, dim), 1) < qk
    loads[3].wait()
    gain = gain_ref[...]

    def attend(i, width, g):
        start = i * local if isinstance(i, int) else pl.multiple_of(i * local, local)
        query = gq[g, pl.ds(start, local)] * BF16(qk ** -0.5)
        zero = jnp.zeros_like(query)
        both = jnp.concatenate([jnp.where(lower, query, zero), jnp.where(lower, zero, query)], 0)
        scores = lax.dot_general(
            both, gk[g, :width], (((1,), (1,)), ((), ())), preferred_element_type=F32
        )
        row = lax.rem(lax.broadcasted_iota(jnp.int32, scores.shape, 0), local)
        col = lax.broadcasted_iota(jnp.int32, scores.shape, 1)
        visible = col // SEGMENT <= (start + row) // SEGMENT
        scores = jnp.where(visible, scores, -jnp.inf)
        raised = jnp.exp(scores - jnp.max(scores, axis=-1, keepdims=True))
        total = jnp.sum(raised, axis=-1, keepdims=True)
        part = jnp.dot(raised.astype(BF16), gv[g, :width], preferred_element_type=F32)
        part = part / total
        attended = part[:local] - hw_ref[g] * part[local:]
        square = jnp.mean(attended * attended, axis=-1, keepdims=True)
        made[i, g] = (attended * lax.rsqrt(square + 1e-06) * gain).astype(BF16)

    def finish(i):
        @pl.when(me != i)
        def _():
            give(i).start()

        @pl.when(me == i)
        def _():
            for g in range(mine):
                back[me * mine + g] = made[i, g]

    if n <= UNROLL:
        for i in range(n):
            arrive(i)
            for g in range(mine):
                attend(i, (i + 1) * local, g)
            finish(i)
    else:
        for j in range(n):
            arrive(j)

        def body(i, carry):
            for g in range(mine):
                attend(i, n * local, g)
            finish(i)
            return carry

        lax.fori_loop(0, n, body, 0)

    for p in peers:
        pltpu.make_async_remote_copy(
            src_ref=made.at[p],
            dst_ref=back.at[pl.ds(p * mine, mine)],
            send_sem=osend_sem.at[p],
            recv_sem=orecv_sem.at[p],
            device_id=there(p),
            device_id_type=pl.DeviceIdType.MESH,
        ).wait_recv()
    for p in peers:
        for t in range(3):
            push(t, p).wait_send()
        give(p).wait_send()


def interleave(heads, local, back_ref, out_ref):
    tokens = max(16, 256 // heads)
    chunk = tokens * heads
    order = order_matrix(chunk, heads, tokens, True)
    for c in range(local // tokens):
        piece = jnp.concatenate(
            [back_ref[h, c * tokens:(c + 1) * tokens] for h in range(heads)], 0
        )
        out_ref[c * chunk:(c + 1) * chunk] = jnp.dot(
            order, piece, preferred_element_type=F32
        ).astype(BF16)


def on_device(n, query_rows, key_rows, value_rows, map_weight, head_gain):
    _, local, heads, dim = query_rows.shape
    mine = heads // n
    flat = (local * heads, dim)
    whole = n * local
    out = pl.pallas_call(
        functools.partial(kernel, n, heads, local, dim // 2),
        out_shape=pltpu.VMEM((heads, local, dim), BF16),
        in_specs=[pl.BlockSpec(memory_space=pltpu.SMEM)]
        + [pl.BlockSpec(memory_space=pltpu.HBM)] * 4,
        out_specs=pl.BlockSpec(memory_space=pltpu.VMEM),
        scratch_shapes=[
            pltpu.VMEM((3,) + flat, BF16),
            pltpu.VMEM((3, heads, local, dim), BF16),
            pltpu.VMEM((mine, whole, dim), BF16),
            pltpu.VMEM((mine, whole, dim), BF16),
            pltpu.VMEM((mine, whole, dim), BF16),
            pltpu.VMEM((n, mine, local, dim), BF16),
            pltpu.VMEM((1, dim), F32),
            pltpu.SemaphoreType.DMA((4,)),
            pltpu.SemaphoreType.DMA((3, n)),
            pltpu.SemaphoreType.DMA((3, n)),
            pltpu.SemaphoreType.DMA((n,)),
            pltpu.SemaphoreType.DMA((n,)),
        ],
        compiler_params=pltpu.CompilerParams(collective_id=0, has_side_effects=True),
    )(
        map_weight,
        head_gain.reshape(1, dim),
        query_rows.reshape(flat),
        key_rows.reshape(flat),
        value_rows.reshape(flat),
    )
    rows = pl.pallas_call(
        functools.partial(interleave, heads, local),
        out_shape=jax.ShapeDtypeStruct(flat, BF16),
        in_specs=[pl.BlockSpec(memory_space=pltpu.VMEM)],
        out_specs=pl.BlockSpec(memory_space=pltpu.VMEM),
        compiler_params=pltpu.CompilerParams(vmem_limit_bytes=KERNEL_BYTES),
    )(out)
    return rows.reshape(query_rows.shape)


def solution(mesh):
    rows = P("dp", "sp", None, None)
    return jax.shard_map(
        functools.partial(on_device, mesh.shape["sp"]),
        mesh=mesh,
        in_specs=(rows, rows, rows, P("sp"), P()),
        out_specs=rows,
        check_vma=False,
    )
```

```python
import functools

import jax
import jax.numpy as jnp
from jax import lax
from jax.experimental import pallas as pl
from jax.experimental.pallas import tpu as pltpu
from jax.sharding import PartitionSpec as P

SEGMENT = 64
CORES = 2
UNROLL = 4
KERNEL_BYTES = 32 * 1024 * 1024
F32 = jnp.float32
BF16 = jnp.bfloat16


def order_matrix(rows, heads, tokens, back):
    out = lax.broadcasted_iota(jnp.int32, (rows, rows), 0)
    src = lax.broadcasted_iota(jnp.int32, (rows, rows), 1)
    if back:
        out, src = src, out
    wanted = (out % tokens) * heads + out // tokens
    return jnp.where(src == wanted, 1.0, 0.0).astype(BF16)


def kernel(
    n, heads, local, qk, hw_ref, gain_hbm, q_hbm, k_hbm, v_hbm, back,
    rows_in, staged, gq, gk, gv, made, gain_ref, in_sem, send_sem, recv_sem, osend_sem, orecv_sem,
):
    dim = q_hbm.shape[-1]
    mine = heads // n
    me = lax.axis_index("sp")
    tokens = max(16, 256 // heads)
    chunk = tokens * heads

    def there(p):
        return {"sp": p}

    sources = (k_hbm, v_hbm, q_hbm)
    loads = [pltpu.make_async_copy(sources[t], rows_in.at[t], in_sem.at[t]) for t in range(3)]
    loads.append(pltpu.make_async_copy(gain_hbm, gain_ref, in_sem.at[3]))
    for load in loads:
        load.start()
    barrier = pltpu.get_barrier_semaphore()
    for d in range(1, n):
        pl.semaphore_signal(
            barrier, inc=1, device_id=there(lax.rem(me + d, n)),
            device_id_type=pl.DeviceIdType.MESH,
        )
    order = order_matrix(chunk, heads, tokens, False)
    gathered = (gk, gv, gq)
    here = pl.ds(pl.multiple_of(me * local, local), local)

    def push(t, p):
        return pltpu.make_async_remote_copy(
            src_ref=staged.at[t, pl.ds(p * mine, mine)],
            dst_ref=gathered[t].at[:, here],
            send_sem=send_sem.at[t, p],
            recv_sem=recv_sem.at[t, me],
            device_id=there(p),
            device_id_type=pl.DeviceIdType.MESH,
        )

    base = (me // CORES) * CORES
    peers = [lax.rem(base + d, n) for d in range(CORES, n)]
    peers += [base + lax.rem(me - base + d, CORES) for d in range(1, CORES)]
    for t in range(3):
        loads[t].wait()
        for c in range(local // tokens):
            moved = jnp.dot(
                order, rows_in[t, c * chunk:(c + 1) * chunk], preferred_element_type=F32
            ).astype(BF16)
            for h in range(heads):
                staged[t, h, c * tokens:(c + 1) * tokens] = moved[h * tokens:(h + 1) * tokens]
        if t == 0:
            pl.semaphore_wait(barrier, n - 1)
        push(t, peers[0]).start()
        for p in peers[n - CORES:]:
            push(t, p).start()
    for p in peers[1:n - CORES]:
        for t in range(3):
            push(t, p).start()
    for t in range(3):
        for g in range(mine):
            gathered[t][g, here] = staged[t, me * mine + g]

    def arrive(j):
        @pl.when(me != j)
        def _():
            for t in range(3):
                pltpu.make_async_remote_copy(
                    src_ref=staged.at[t, pl.ds(0, mine)],
                    dst_ref=gathered[t].at[:, pl.ds(pl.multiple_of(j * local, local), local)],
                    send_sem=send_sem.at[t, j],
                    recv_sem=recv_sem.at[t, j],
                    device_id=there(j),
                    device_id_type=pl.DeviceIdType.MESH,
                ).wait_recv()

    def give(i):
        return pltpu.make_async_remote_copy(
            src_ref=made.at[i],
            dst_ref=back.at[pl.ds(me * mine, mine)],
            send_sem=osend_sem.at[i],
            recv_sem=orecv_sem.at[me],
            device_id=there(i),
            device_id_type=pl.DeviceIdType.MESH,
        )

    lower = lax.broadcasted_iota(jnp.int32, (local, dim), 1) < qk
    loads[3].wait()
    gain = gain_ref[...]

    def attend(i, width, g):
        start = i * local if isinstance(i, int) else pl.multiple_of(i * local, local)
        query = gq[g, pl.ds(start, local)] * BF16(qk ** -0.5)
        zero = jnp.zeros_like(query)
        both = jnp.concatenate([jnp.where(lower, query, zero), jnp.where(lower, zero, query)], 0)
        scores = lax.dot_general(
            both, gk[g, :width], (((1,), (1,)), ((), ())), preferred_element_type=F32
        )
        row = lax.rem(lax.broadcasted_iota(jnp.int32, scores.shape, 0), local)
        col = lax.broadcasted_iota(jnp.int32, scores.shape, 1)
        visible = col // SEGMENT <= (start + row) // SEGMENT
        scores = jnp.where(visible, scores, -jnp.inf)
        raised = jnp.exp(scores - jnp.max(scores, axis=-1, keepdims=True))
        total = jnp.sum(raised, axis=-1, keepdims=True)
        part = jnp.dot(raised.astype(BF16), gv[g, :width], preferred_element_type=F32)
        part = part / total
        attended = part[:local] - hw_ref[g] * part[local:]
        square = jnp.mean(attended * attended, axis=-1, keepdims=True)
        made[i, g] = (attended * lax.rsqrt(square + 1e-06) * gain).astype(BF16)

    def finish(i):
        @pl.when(me != i)
        def _():
            give(i).start()

        @pl.when(me == i)
        def _():
            for g in range(mine):
                back[me * mine + g] = made[i, g]

    if n <= UNROLL:
        for i in range(n):
            arrive(i)
            for g in range(mine):
                attend(i, (i + 1) * local, g)
            finish(i)
    else:
        for j in range(n):
            arrive(j)

        def body(i, carry):
            for g in range(mine):
                attend(i, n * local, g)
            finish(i)
            return carry

        lax.fori_loop(0, n, body, 0)

    for p in peers:
        pltpu.make_async_remote_copy(
            src_ref=made.at[p],
            dst_ref=back.at[pl.ds(p * mine, mine)],
            send_sem=osend_sem.at[p],
            recv_sem=orecv_sem.at[p],
            device_id=there(p),
            device_id_type=pl.DeviceIdType.MESH,
        ).wait_recv()
    for p in peers:
        for t in range(3):
            push(t, p).wait_send()
        give(p).wait_send()


def pair_kernel(
    heads, local, qk, hw_ref, gain_hbm, q_hbm, k_hbm, v_hbm, back,
    rows_in, gq, gk, gv, lent, made, gain_ref, weight, in_sem, wsend_sem, wrecv_sem,
    send_sem, recv_sem, qsend_sem, qrecv_sem, osend_sem, orecv_sem,
):
    dim = q_hbm.shape[-1]
    moved = heads // 4
    me = lax.axis_index("sp")
    tokens = max(16, 256 // heads)
    chunk = tokens * heads
    across = lax.rem(me + CORES, 2 * CORES)
    beside = me + 1 - 2 * lax.rem(me, CORES)
    gathered = (gk, gv)

    loads = [
        pltpu.make_async_copy(src, rows_in.at[t], in_sem.at[t])
        for t, src in enumerate((k_hbm, v_hbm, q_hbm))
    ]
    loads.append(pltpu.make_async_copy(gain_hbm, gain_ref, in_sem.at[3]))
    for load in loads:
        load.start()
    barrier = pltpu.get_barrier_semaphore()
    others = [lax.rem(me + d, 2 * CORES) for d in range(1, 2 * CORES)]
    for p in others:
        pl.semaphore_signal(
            barrier, inc=1, device_id={"sp": p}, device_id_type=pl.DeviceIdType.MESH
        )
    mine = heads // (2 * CORES)
    for g in range(mine):
        weight[me * mine + g] = jnp.full((8, dim), hw_ref[g], F32)

    def tell(p, j):
        rows = weight.at[pl.ds(j * mine, mine)]
        return pltpu.make_async_remote_copy(
            src_ref=rows, dst_ref=rows,
            send_sem=wsend_sem.at[p], recv_sem=wrecv_sem.at[j],
            device_id={"sp": p}, device_id_type=pl.DeviceIdType.MESH,
        )

    order = order_matrix(chunk, heads, tokens, False)

    def relay(t):
        loads[t].wait()
        for c in range(local // tokens):
            rows = jnp.dot(
                order, rows_in[t, c * chunk:(c + 1) * chunk], preferred_element_type=F32
            ).astype(BF16)
            for h in range(heads):
                piece = rows[h * tokens:(h + 1) * tokens]
                if t == 2:
                    gq[h, c * tokens:(c + 1) * tokens] = piece
                else:
                    start = pl.multiple_of(me * local + c * tokens, tokens)
                    gathered[t][h, pl.ds(start, tokens)] = piece

    def block(t, h, j):
        start = j * local if isinstance(j, int) else pl.multiple_of(j * local, local)
        return gathered[t].at[h, pl.ds(start, local)]

    def move(t, h, j, p, kind):
        return pltpu.make_async_remote_copy(
            src_ref=block(t, h, j),
            dst_ref=block(t, h, j),
            send_sem=send_sem.at[kind, t, h, j],
            recv_sem=recv_sem.at[t, h, j],
            device_id={"sp": p},
            device_id_type=pl.DeviceIdType.MESH,
        )

    def lend(h, p):
        return pltpu.make_async_remote_copy(
            src_ref=gq.at[h], dst_ref=lent.at[h],
            send_sem=qsend_sem.at[h], recv_sem=qrecv_sem.at[h],
            device_id={"sp": p}, device_id_type=pl.DeviceIdType.MESH,
        )

    def give(h, p):
        return pltpu.make_async_remote_copy(
            src_ref=made.at[h], dst_ref=back.at[h],
            send_sem=osend_sem.at[h], recv_sem=orecv_sem.at[h],
            device_id={"sp": p}, device_id_type=pl.DeviceIdType.MESH,
        )

    relay(0)
    pl.semaphore_wait(barrier, 2 * CORES - 1)
    for p in others:
        tell(p, me).start()

    @pl.when(me < CORES)
    def _():
        move(0, moved, me, across, 0).start()

    @pl.when(me >= CORES)
    def _():
        move(0, 0, me, across, 0).start()

    relay(1)
    relay(2)
    loads[3].wait()
    gain = gain_ref[...]
    lower = lax.broadcasted_iota(jnp.int32, (local, dim), 1) < qk
    row = lax.rem(lax.broadcasted_iota(jnp.int32, (2 * local, local), 0), local)
    col = lax.broadcasted_iota(jnp.int32, (2 * local, local), 1)
    visible = col // SEGMENT <= row // SEGMENT

    def weigh(query, h, i):
        query = query * BF16(qk ** -0.5)
        zero = jnp.zeros_like(query)
        both = jnp.concatenate([jnp.where(lower, query, zero), jnp.where(lower, zero, query)], 0)
        across_dim = (((1,), (1,)), ((), ()))
        scores = lax.dot_general(
            both, gk[h, i * local:(i + 1) * local], across_dim, preferred_element_type=F32
        )
        scores = jnp.where(visible, scores, -jnp.inf)
        if i:
            past = lax.dot_general(
                both, gk[h, :i * local], across_dim, preferred_element_type=F32
            )
            scores = jnp.concatenate([past, scores], 1)
        raised = jnp.exp(scores - jnp.max(scores, axis=-1, keepdims=True))
        return raised.astype(BF16), jnp.sum(raised, axis=-1, keepdims=True)

    def mix(raised, total, h, i):
        part = jnp.dot(raised, gv[h, :(i + 1) * local], preferred_element_type=F32)
        part = part / total
        attended = part[:local] - weight[h, 0:1] * part[local:]
        square = jnp.mean(attended * attended, axis=-1, keepdims=True)
        return (attended * lax.rsqrt(square + 1e-06) * gain).astype(BF16)

    def role(r):
        side, other = r + 1 - 2 * (r % CORES), (r + CORES) % (2 * CORES)
        sent = []

        def go(copy, begun=False):
            if not begun:
                copy.start()
            sent.append(copy)

        def hear():
            for p in range(2 * CORES):
                if p != r:
                    tell(p, p).wait_recv()

        def landed(t, h, j):
            move(t, h, j, side, 1).wait_recv()

        def pass_on(t, h, j):
            landed(t, h, j)
            go(move(t, h, j, side, 1))

        if r < CORES:
            for h in range(moved, heads):
                for t in range(2):
                    go(move(t, h, r, other, 0), begun=(h == moved and t == 0))
            for h in range(heads if r == 0 else moved):
                for t in range(2):
                    go(move(t, h, r, side, 1))
            hear()
            for h in range(heads):
                if r:
                    landed(0, h, 0)
                    landed(1, h, 0)
                back[h] = mix(*weigh(gq[h], h, r), h, r)
            for h in range(moved):
                if r == 0:
                    pass_on(0, h, other)
                    pass_on(1, h, other)
                    landed(0, h, 1)
                    landed(1, h, 1)
                else:
                    landed(0, h, other)
                    landed(0, h, other - 1)
                lend(h, other).wait_recv()
                weights = weigh(lent[h], h, other)
                if r:
                    landed(1, h, other)
                    landed(1, h, other - 1)
                made[h] = mix(*weights, h, other)
                go(give(h, other))
        else:
            for h in range(moved):
                for t in range(2):
                    go(move(t, h, r, other, 0), begun=(h == 0 and t == 0))
                go(lend(h, other))
            if r == CORES:
                for h in range(moved, heads):
                    for t in range(2):
                        go(move(t, h, r, side, 1))
            hear()
            far = side - CORES
            pass_on(0, moved, other)
            for h in range(moved, heads):
                pass_on(1, h, other)
                if h + 1 < heads:
                    pass_on(0, h + 1, other)
                landed(0, h, far)
                if r > CORES:
                    landed(0, h, side)
                weights = weigh(gq[h], h, r)
                landed(1, h, far)
                if r > CORES:
                    landed(1, h, side)
                back[h] = mix(*weights, h, r)
            for h in range(moved):
                give(h, other).wait_recv()
        for copy in sent:
            copy.wait_send()

    for r in range(2 * CORES):
        pl.when(me == r)(functools.partial(role, r))
    for p in others:
        tell(p, me).wait_send()


def interleave(heads, local, back_ref, out_ref):
    tokens = max(16, 256 // heads)
    chunk = tokens * heads
    order = order_matrix(chunk, heads, tokens, True)
    for c in range(local // tokens):
        piece = jnp.concatenate(
            [back_ref[h, c * tokens:(c + 1) * tokens] for h in range(heads)], 0
        )
        out_ref[c * chunk:(c + 1) * chunk] = jnp.dot(
            order, piece, preferred_element_type=F32
        ).astype(BF16)


def on_device(n, query_rows, key_rows, value_rows, map_weight, head_gain):
    _, local, heads, dim = query_rows.shape
    mine = heads // n
    flat = (local * heads, dim)
    whole = n * local
    paired = n == 2 * CORES and heads % 4 == 0
    if paired:
        moved = heads // 4
        body = functools.partial(pair_kernel, heads, local, dim // 2)
        scratch = [
            pltpu.VMEM((heads, local, dim), BF16),
            pltpu.VMEM((heads, whole, dim), BF16),
            pltpu.VMEM((heads, whole, dim), BF16),
            pltpu.VMEM((moved, local, dim), BF16),
            pltpu.VMEM((moved, local, dim), BF16),
            pltpu.VMEM((1, dim), F32),
            pltpu.VMEM((heads, 8, dim), F32),
            pltpu.SemaphoreType.DMA((4,)),
            pltpu.SemaphoreType.DMA((n,)),
            pltpu.SemaphoreType.DMA((n,)),
            pltpu.SemaphoreType.DMA((2, 2, heads, n)),
            pltpu.SemaphoreType.DMA((2, heads, n)),
        ] + [pltpu.SemaphoreType.DMA((moved,))] * 4
    else:
        body = functools.partial(kernel, n, heads, local, dim // 2)
        scratch = [
            pltpu.VMEM((3, heads, local, dim), BF16),
            pltpu.VMEM((mine, whole, dim), BF16),
            pltpu.VMEM((mine, whole, dim), BF16),
            pltpu.VMEM((mine, whole, dim), BF16),
            pltpu.VMEM((n, mine, local, dim), BF16),
            pltpu.VMEM((1, dim), F32),
            pltpu.SemaphoreType.DMA((4,)),
            pltpu.SemaphoreType.DMA((3, n)),
            pltpu.SemaphoreType.DMA((3, n)),
            pltpu.SemaphoreType.DMA((n,)),
            pltpu.SemaphoreType.DMA((n,)),
        ]
    out = pl.pallas_call(
        body,
        out_shape=pltpu.VMEM((heads, local, dim), BF16),
        in_specs=[pl.BlockSpec(memory_space=pltpu.SMEM)]
        + [pl.BlockSpec(memory_space=pltpu.HBM)] * 4,
        out_specs=pl.BlockSpec(memory_space=pltpu.VMEM),
        scratch_shapes=[pltpu.VMEM((3,) + flat, BF16)] + scratch,
        compiler_params=pltpu.CompilerParams(collective_id=0, has_side_effects=True),
    )(
        map_weight,
        head_gain.reshape(1, dim),
        query_rows.reshape(flat),
        key_rows.reshape(flat),
        value_rows.reshape(flat),
    )
    rows = pl.pallas_call(
        functools.partial(interleave, heads, local),
        out_shape=jax.ShapeDtypeStruct(flat, BF16),
        in_specs=[pl.BlockSpec(memory_space=pltpu.VMEM)],
        out_specs=pl.BlockSpec(memory_space=pltpu.VMEM),
        compiler_params=pltpu.CompilerParams(vmem_limit_bytes=KERNEL_BYTES),
    )(out)
    return rows.reshape(query_rows.shape)


def solution(mesh):
    rows = P("dp", "sp", None, None)
    return jax.shard_map(
        functools.partial(on_device, mesh.shape["sp"]),
        mesh=mesh,
        in_specs=(rows, rows, rows, P("sp"), P()),
        out_specs=rows,
        check_vma=False,
    )
```

```python
import functools

import jax
import jax.numpy as jnp
from jax import lax
from jax.experimental import pallas as pl
from jax.experimental.pallas import tpu as pltpu
from jax.sharding import PartitionSpec as P

SEGMENT = 64
CORES = 2
UNROLL = 4
KERNEL_BYTES = 32 * 1024 * 1024
F32 = jnp.float32
BF16 = jnp.bfloat16


def order_matrix(rows, heads, tokens, back):
    out = lax.broadcasted_iota(jnp.int32, (rows, rows), 0)
    src = lax.broadcasted_iota(jnp.int32, (rows, rows), 1)
    if back:
        out, src = src, out
    wanted = (out % tokens) * heads + out // tokens
    return jnp.where(src == wanted, 1.0, 0.0).astype(BF16)


def kernel(
    n, heads, local, qk, hw_ref, gain_hbm, q_hbm, k_hbm, v_hbm, back,
    rows_in, staged, gq, gk, gv, made, gain_ref, in_sem, send_sem, recv_sem, osend_sem, orecv_sem,
):
    dim = q_hbm.shape[-1]
    mine = heads // n
    me = lax.axis_index("sp")
    tokens = max(16, 256 // heads)
    chunk = tokens * heads

    def there(p):
        return {"sp": p}

    sources = (k_hbm, v_hbm, q_hbm)
    loads = [pltpu.make_async_copy(sources[t], rows_in.at[t], in_sem.at[t]) for t in range(3)]
    loads.append(pltpu.make_async_copy(gain_hbm, gain_ref, in_sem.at[3]))
    for load in loads:
        load.start()
    barrier = pltpu.get_barrier_semaphore()
    for d in range(1, n):
        pl.semaphore_signal(
            barrier, inc=1, device_id=there(lax.rem(me + d, n)),
            device_id_type=pl.DeviceIdType.MESH,
        )
    order = order_matrix(chunk, heads, tokens, False)
    gathered = (gk, gv, gq)
    here = pl.ds(pl.multiple_of(me * local, local), local)

    def push(t, p):
        return pltpu.make_async_remote_copy(
            src_ref=staged.at[t, pl.ds(p * mine, mine)],
            dst_ref=gathered[t].at[:, here],
            send_sem=send_sem.at[t, p],
            recv_sem=recv_sem.at[t, me],
            device_id=there(p),
            device_id_type=pl.DeviceIdType.MESH,
        )

    base = (me // CORES) * CORES
    peers = [lax.rem(base + d, n) for d in range(CORES, n)]
    peers += [base + lax.rem(me - base + d, CORES) for d in range(1, CORES)]
    for t in range(3):
        loads[t].wait()
        for c in range(local // tokens):
            moved = jnp.dot(
                order, rows_in[t, c * chunk:(c + 1) * chunk], preferred_element_type=F32
            ).astype(BF16)
            for h in range(heads):
                staged[t, h, c * tokens:(c + 1) * tokens] = moved[h * tokens:(h + 1) * tokens]
        if t == 0:
            pl.semaphore_wait(barrier, n - 1)
        push(t, peers[0]).start()
        for p in peers[n - CORES:]:
            push(t, p).start()
    for p in peers[1:n - CORES]:
        for t in range(3):
            push(t, p).start()
    for t in range(3):
        for g in range(mine):
            gathered[t][g, here] = staged[t, me * mine + g]

    def arrive(j):
        @pl.when(me != j)
        def _():
            for t in range(3):
                pltpu.make_async_remote_copy(
                    src_ref=staged.at[t, pl.ds(0, mine)],
                    dst_ref=gathered[t].at[:, pl.ds(pl.multiple_of(j * local, local), local)],
                    send_sem=send_sem.at[t, j],
                    recv_sem=recv_sem.at[t, j],
                    device_id=there(j),
                    device_id_type=pl.DeviceIdType.MESH,
                ).wait_recv()

    def give(i):
        return pltpu.make_async_remote_copy(
            src_ref=made.at[i],
            dst_ref=back.at[pl.ds(me * mine, mine)],
            send_sem=osend_sem.at[i],
            recv_sem=orecv_sem.at[me],
            device_id=there(i),
            device_id_type=pl.DeviceIdType.MESH,
        )

    lower = lax.broadcasted_iota(jnp.int32, (local, dim), 1) < qk
    loads[3].wait()
    gain = gain_ref[...]

    def attend(i, width, g):
        start = i * local if isinstance(i, int) else pl.multiple_of(i * local, local)
        query = gq[g, pl.ds(start, local)] * BF16(qk ** -0.5)
        zero = jnp.zeros_like(query)
        both = jnp.concatenate([jnp.where(lower, query, zero), jnp.where(lower, zero, query)], 0)
        scores = lax.dot_general(
            both, gk[g, :width], (((1,), (1,)), ((), ())), preferred_element_type=F32
        )
        row = lax.rem(lax.broadcasted_iota(jnp.int32, scores.shape, 0), local)
        col = lax.broadcasted_iota(jnp.int32, scores.shape, 1)
        visible = col // SEGMENT <= (start + row) // SEGMENT
        scores = jnp.where(visible, scores, -jnp.inf)
        raised = jnp.exp(scores - jnp.max(scores, axis=-1, keepdims=True))
        total = jnp.sum(raised, axis=-1, keepdims=True)
        part = jnp.dot(raised.astype(BF16), gv[g, :width], preferred_element_type=F32)
        part = part / total
        attended = part[:local] - hw_ref[g] * part[local:]
        square = jnp.mean(attended * attended, axis=-1, keepdims=True)
        made[i, g] = (attended * lax.rsqrt(square + 1e-06) * gain).astype(BF16)

    def finish(i):
        @pl.when(me != i)
        def _():
            give(i).start()

        @pl.when(me == i)
        def _():
            for g in range(mine):
                back[me * mine + g] = made[i, g]

    if n <= UNROLL:
        for i in range(n):
            arrive(i)
            for g in range(mine):
                attend(i, (i + 1) * local, g)
            finish(i)
    else:
        for j in range(n):
            arrive(j)

        def body(i, carry):
            for g in range(mine):
                attend(i, n * local, g)
            finish(i)
            return carry

        lax.fori_loop(0, n, body, 0)

    for p in peers:
        pltpu.make_async_remote_copy(
            src_ref=made.at[p],
            dst_ref=back.at[pl.ds(p * mine, mine)],
            send_sem=osend_sem.at[p],
            recv_sem=orecv_sem.at[p],
            device_id=there(p),
            device_id_type=pl.DeviceIdType.MESH,
        ).wait_recv()
    for p in peers:
        for t in range(3):
            push(t, p).wait_send()
        give(p).wait_send()


def pair_kernel(
    heads, local, qk, hw_ref, gain_hbm, q_hbm, k_hbm, v_hbm, back,
    rows_in, gq, gk, gv, lent, made, gain_ref, weight, in_sem, wsend_sem, wrecv_sem,
    send_sem, recv_sem, qsend_sem, qrecv_sem, osend_sem, orecv_sem,
):
    dim = q_hbm.shape[-1]
    moved = heads // 4
    me = lax.axis_index("sp")
    tokens = max(16, 256 // heads)
    chunk = tokens * heads
    across = 2 * CORES - 1 - me
    beside = me + 1 - 2 * lax.rem(me, CORES)
    gathered = (gk, gv)

    loads = [
        pltpu.make_async_copy(src, rows_in.at[t], in_sem.at[t])
        for t, src in enumerate((k_hbm, v_hbm, q_hbm))
    ]
    loads.append(pltpu.make_async_copy(gain_hbm, gain_ref, in_sem.at[3]))
    for load in loads:
        load.start()
    barrier = pltpu.get_barrier_semaphore()
    others = [lax.rem(me + d, 2 * CORES) for d in range(1, 2 * CORES)]
    for p in others:
        pl.semaphore_signal(
            barrier, inc=1, device_id={"sp": p}, device_id_type=pl.DeviceIdType.MESH
        )
    mine = heads // (2 * CORES)
    for g in range(mine):
        weight[me * mine + g] = jnp.full((8, dim), hw_ref[g], F32)

    def tell(p, j):
        rows = weight.at[pl.ds(j * mine, mine)]
        return pltpu.make_async_remote_copy(
            src_ref=rows, dst_ref=rows,
            send_sem=wsend_sem.at[p], recv_sem=wrecv_sem.at[j],
            device_id={"sp": p}, device_id_type=pl.DeviceIdType.MESH,
        )

    order = order_matrix(chunk, heads, tokens, False)

    def relay(t):
        loads[t].wait()
        for c in range(local // tokens):
            rows = jnp.dot(
                order, rows_in[t, c * chunk:(c + 1) * chunk], preferred_element_type=F32
            ).astype(BF16)
            for h in range(heads):
                piece = rows[h * tokens:(h + 1) * tokens]
                if t == 2:
                    gq[h, c * tokens:(c + 1) * tokens] = piece
                else:
                    start = pl.multiple_of(me * local + c * tokens, tokens)
                    gathered[t][h, pl.ds(start, tokens)] = piece

    def block(t, h, j):
        start = j * local if isinstance(j, int) else pl.multiple_of(j * local, local)
        return gathered[t].at[h, pl.ds(start, local)]

    def move(t, h, j, p, kind):
        return pltpu.make_async_remote_copy(
            src_ref=block(t, h, j),
            dst_ref=block(t, h, j),
            send_sem=send_sem.at[kind, t, h, j],
            recv_sem=recv_sem.at[t, h, j],
            device_id={"sp": p},
            device_id_type=pl.DeviceIdType.MESH,
        )

    def lend(h, p):
        return pltpu.make_async_remote_copy(
            src_ref=gq.at[h], dst_ref=lent.at[h],
            send_sem=qsend_sem.at[h], recv_sem=qrecv_sem.at[h],
            device_id={"sp": p}, device_id_type=pl.DeviceIdType.MESH,
        )

    def give(h, p):
        return pltpu.make_async_remote_copy(
            src_ref=made.at[h], dst_ref=back.at[h],
            send_sem=osend_sem.at[h], recv_sem=orecv_sem.at[h],
            device_id={"sp": p}, device_id_type=pl.DeviceIdType.MESH,
        )

    relay(0)
    pl.semaphore_wait(barrier, 2 * CORES - 1)
    for p in others:
        tell(p, me).start()

    @pl.when(me < CORES)
    def _():
        move(0, moved, me, across, 0).start()

    @pl.when(me >= CORES)
    def _():
        move(0, 0, me, across, 0).start()

    relay(1)
    relay(2)
    loads[3].wait()
    gain = gain_ref[...]
    lower = lax.broadcasted_iota(jnp.int32, (local, dim), 1) < qk
    row = lax.rem(lax.broadcasted_iota(jnp.int32, (2 * local, local), 0), local)
    col = lax.broadcasted_iota(jnp.int32, (2 * local, local), 1)
    visible = col // SEGMENT <= row // SEGMENT

    def weigh(query, h, i):
        query = query * BF16(qk ** -0.5)
        zero = jnp.zeros_like(query)
        both = jnp.concatenate([jnp.where(lower, query, zero), jnp.where(lower, zero, query)], 0)
        across_dim = (((1,), (1,)), ((), ()))
        scores = lax.dot_general(
            both, gk[h, i * local:(i + 1) * local], across_dim, preferred_element_type=F32
        )
        scores = jnp.where(visible, scores, -jnp.inf)
        if i:
            past = lax.dot_general(
                both, gk[h, :i * local], across_dim, preferred_element_type=F32
            )
            scores = jnp.concatenate([past, scores], 1)
        raised = jnp.exp(scores - jnp.max(scores, axis=-1, keepdims=True))
        return raised.astype(BF16), jnp.sum(raised, axis=-1, keepdims=True)

    def mix(raised, total, h, i):
        part = jnp.dot(raised, gv[h, :(i + 1) * local], preferred_element_type=F32)
        part = part / total
        attended = part[:local] - weight[h, 0:1] * part[local:]
        square = jnp.mean(attended * attended, axis=-1, keepdims=True)
        return (attended * lax.rsqrt(square + 1e-06) * gain).astype(BF16)

    def role(r):
        side, other = r + 1 - 2 * (r % CORES), 2 * CORES - 1 - r
        sent = []

        def go(copy, begun=False):
            if not begun:
                copy.start()
            sent.append(copy)

        def hear():
            for p in range(2 * CORES):
                if p != r:
                    tell(p, p).wait_recv()

        def landed(t, h, j):
            move(t, h, j, side, 1).wait_recv()

        def pass_on(t, h, j):
            landed(t, h, j)
            go(move(t, h, j, side, 1))

        if r < CORES:
            for h in range(moved, heads):
                for t in range(2):
                    go(move(t, h, r, other, 0), begun=(h == moved and t == 0))
            for h in range(heads if r == 0 else moved):
                for t in range(2):
                    go(move(t, h, r, side, 1))
            hear()
            for h in range(heads):
                if r:
                    landed(0, h, 0)
                    landed(1, h, 0)
                back[h] = mix(*weigh(gq[h], h, r), h, r)
            for h in range(moved):
                if r:
                    pass_on(0, h, other)
                    pass_on(1, h, other)
                else:
                    landed(0, h, 1)
                    landed(1, h, 1)
                    landed(0, h, other - 1)
                    landed(0, h, other)
                lend(h, other).wait_recv()
                weights = weigh(lent[h], h, other)
                if r == 0:
                    landed(1, h, other - 1)
                    landed(1, h, other)
                made[h] = mix(*weights, h, other)
                go(give(h, other))
        else:
            for h in range(moved):
                for t in range(2):
                    go(move(t, h, r, other, 0), begun=(h == 0 and t == 0))
                go(lend(h, other))
            if r == CORES:
                for h in range(moved, heads):
                    for t in range(2):
                        go(move(t, h, r, side, 1))
            hear()
            far = CORES - 1 - other
            pass_on(0, moved, other)
            for h in range(moved, heads):
                pass_on(1, h, other)
                if h + 1 < heads:
                    pass_on(0, h + 1, other)
                landed(0, h, far)
                if r > CORES:
                    landed(0, h, side)
                weights = weigh(gq[h], h, r)
                landed(1, h, far)
                if r > CORES:
                    landed(1, h, side)
                back[h] = mix(*weights, h, r)
            for h in range(moved):
                give(h, other).wait_recv()
        for copy in sent:
            copy.wait_send()

    for r in range(2 * CORES):
        pl.when(me == r)(functools.partial(role, r))
    for p in others:
        tell(p, me).wait_send()


def interleave(heads, local, back_ref, out_ref):
    tokens = max(16, 256 // heads)
    chunk = tokens * heads
    order = order_matrix(chunk, heads, tokens, True)
    for c in range(local // tokens):
        piece = jnp.concatenate(
            [back_ref[h, c * tokens:(c + 1) * tokens] for h in range(heads)], 0
        )
        out_ref[c * chunk:(c + 1) * chunk] = jnp.dot(
            order, piece, preferred_element_type=F32
        ).astype(BF16)


def on_device(n, query_rows, key_rows, value_rows, map_weight, head_gain):
    _, local, heads, dim = query_rows.shape
    mine = heads // n
    flat = (local * heads, dim)
    whole = n * local
    paired = n == 2 * CORES and heads % 4 == 0
    if paired:
        moved = heads // 4
        body = functools.partial(pair_kernel, heads, local, dim // 2)
        scratch = [
            pltpu.VMEM((heads, local, dim), BF16),
            pltpu.VMEM((heads, whole, dim), BF16),
            pltpu.VMEM((heads, whole, dim), BF16),
            pltpu.VMEM((moved, local, dim), BF16),
            pltpu.VMEM((moved, local, dim), BF16),
            pltpu.VMEM((1, dim), F32),
            pltpu.VMEM((heads, 8, dim), F32),
            pltpu.SemaphoreType.DMA((4,)),
            pltpu.SemaphoreType.DMA((n,)),
            pltpu.SemaphoreType.DMA((n,)),
            pltpu.SemaphoreType.DMA((2, 2, heads, n)),
            pltpu.SemaphoreType.DMA((2, heads, n)),
        ] + [pltpu.SemaphoreType.DMA((moved,))] * 4
    else:
        body = functools.partial(kernel, n, heads, local, dim // 2)
        scratch = [
            pltpu.VMEM((3, heads, local, dim), BF16),
            pltpu.VMEM((mine, whole, dim), BF16),
            pltpu.VMEM((mine, whole, dim), BF16),
            pltpu.VMEM((mine, whole, dim), BF16),
            pltpu.VMEM((n, mine, local, dim), BF16),
            pltpu.VMEM((1, dim), F32),
            pltpu.SemaphoreType.DMA((4,)),
            pltpu.SemaphoreType.DMA((3, n)),
            pltpu.SemaphoreType.DMA((3, n)),
            pltpu.SemaphoreType.DMA((n,)),
            pltpu.SemaphoreType.DMA((n,)),
        ]
    out = pl.pallas_call(
        body,
        out_shape=pltpu.VMEM((heads, local, dim), BF16),
        in_specs=[pl.BlockSpec(memory_space=pltpu.SMEM)]
        + [pl.BlockSpec(memory_space=pltpu.HBM)] * 4,
        out_specs=pl.BlockSpec(memory_space=pltpu.VMEM),
        scratch_shapes=[pltpu.VMEM((3,) + flat, BF16)] + scratch,
        compiler_params=pltpu.CompilerParams(collective_id=0, has_side_effects=True),
    )(
        map_weight,
        head_gain.reshape(1, dim),
        query_rows.reshape(flat),
        key_rows.reshape(flat),
        value_rows.reshape(flat),
    )
    rows = pl.pallas_call(
        functools.partial(interleave, heads, local),
        out_shape=jax.ShapeDtypeStruct(flat, BF16),
        in_specs=[pl.BlockSpec(memory_space=pltpu.VMEM)],
        out_specs=pl.BlockSpec(memory_space=pltpu.VMEM),
        compiler_params=pltpu.CompilerParams(vmem_limit_bytes=KERNEL_BYTES),
    )(out)
    return rows.reshape(query_rows.shape)


def solution(mesh):
    rows = P("dp", "sp", None, None)
    return jax.shard_map(
        functools.partial(on_device, mesh.shape["sp"]),
        mesh=mesh,
        in_specs=(rows, rows, rows, P("sp"), P()),
        out_specs=rows,
        check_vma=False,
    )
```

```python
import functools

import jax
import jax.numpy as jnp
from jax import lax
from jax.experimental import pallas as pl
from jax.experimental.pallas import tpu as pltpu
from jax.sharding import PartitionSpec as P

SEGMENT = 64
CORES = 2
UNROLL = 4
KERNEL_BYTES = 32 * 1024 * 1024
F32 = jnp.float32
BF16 = jnp.bfloat16


def order_matrix(rows, heads, tokens, back):
    out = lax.broadcasted_iota(jnp.int32, (rows, rows), 0)
    src = lax.broadcasted_iota(jnp.int32, (rows, rows), 1)
    if back:
        out, src = src, out
    wanted = (out % tokens) * heads + out // tokens
    return jnp.where(src == wanted, 1.0, 0.0).astype(BF16)


def kernel(
    n, heads, local, qk, hw_ref, gain_hbm, q_hbm, k_hbm, v_hbm, back,
    rows_in, staged, gq, gk, gv, made, gain_ref, in_sem, send_sem, recv_sem, osend_sem, orecv_sem,
):
    dim = q_hbm.shape[-1]
    mine = heads // n
    me = lax.axis_index("sp")
    tokens = max(16, 256 // heads)
    chunk = tokens * heads

    def there(p):
        return {"sp": p}

    sources = (k_hbm, v_hbm, q_hbm)
    loads = [pltpu.make_async_copy(sources[t], rows_in.at[t], in_sem.at[t]) for t in range(3)]
    loads.append(pltpu.make_async_copy(gain_hbm, gain_ref, in_sem.at[3]))
    for load in loads:
        load.start()
    barrier = pltpu.get_barrier_semaphore()
    for d in range(1, n):
        pl.semaphore_signal(
            barrier, inc=1, device_id=there(lax.rem(me + d, n)),
            device_id_type=pl.DeviceIdType.MESH,
        )
    order = order_matrix(chunk, heads, tokens, False)
    gathered = (gk, gv, gq)
    here = pl.ds(pl.multiple_of(me * local, local), local)

    def push(t, p):
        return pltpu.make_async_remote_copy(
            src_ref=staged.at[t, pl.ds(p * mine, mine)],
            dst_ref=gathered[t].at[:, here],
            send_sem=send_sem.at[t, p],
            recv_sem=recv_sem.at[t, me],
            device_id=there(p),
            device_id_type=pl.DeviceIdType.MESH,
        )

    base = (me // CORES) * CORES
    peers = [lax.rem(base + d, n) for d in range(CORES, n)]
    peers += [base + lax.rem(me - base + d, CORES) for d in range(1, CORES)]
    for t in range(3):
        loads[t].wait()
        for c in range(local // tokens):
            moved = jnp.dot(
                order, rows_in[t, c * chunk:(c + 1) * chunk], preferred_element_type=F32
            ).astype(BF16)
            for h in range(heads):
                staged[t, h, c * tokens:(c + 1) * tokens] = moved[h * tokens:(h + 1) * tokens]
        if t == 0:
            pl.semaphore_wait(barrier, n - 1)
        push(t, peers[0]).start()
        for p in peers[n - CORES:]:
            push(t, p).start()
    for p in peers[1:n - CORES]:
        for t in range(3):
            push(t, p).start()
    for t in range(3):
        for g in range(mine):
            gathered[t][g, here] = staged[t, me * mine + g]

    def arrive(j):
        @pl.when(me != j)
        def _():
            for t in range(3):
                pltpu.make_async_remote_copy(
                    src_ref=staged.at[t, pl.ds(0, mine)],
                    dst_ref=gathered[t].at[:, pl.ds(pl.multiple_of(j * local, local), local)],
                    send_sem=send_sem.at[t, j],
                    recv_sem=recv_sem.at[t, j],
                    device_id=there(j),
                    device_id_type=pl.DeviceIdType.MESH,
                ).wait_recv()

    def give(i):
        return pltpu.make_async_remote_copy(
            src_ref=made.at[i],
            dst_ref=back.at[pl.ds(me * mine, mine)],
            send_sem=osend_sem.at[i],
            recv_sem=orecv_sem.at[me],
            device_id=there(i),
            device_id_type=pl.DeviceIdType.MESH,
        )

    lower = lax.broadcasted_iota(jnp.int32, (local, dim), 1) < qk
    loads[3].wait()
    gain = gain_ref[...]

    def attend(i, width, g):
        start = i * local if isinstance(i, int) else pl.multiple_of(i * local, local)
        query = gq[g, pl.ds(start, local)] * BF16(qk ** -0.5)
        zero = jnp.zeros_like(query)
        both = jnp.concatenate([jnp.where(lower, query, zero), jnp.where(lower, zero, query)], 0)
        scores = lax.dot_general(
            both, gk[g, :width], (((1,), (1,)), ((), ())), preferred_element_type=F32
        )
        row = lax.rem(lax.broadcasted_iota(jnp.int32, scores.shape, 0), local)
        col = lax.broadcasted_iota(jnp.int32, scores.shape, 1)
        visible = col // SEGMENT <= (start + row) // SEGMENT
        scores = jnp.where(visible, scores, -jnp.inf)
        raised = jnp.exp(scores - jnp.max(scores, axis=-1, keepdims=True))
        total = jnp.sum(raised, axis=-1, keepdims=True)
        part = jnp.dot(raised.astype(BF16), gv[g, :width], preferred_element_type=F32)
        part = part / total
        attended = part[:local] - hw_ref[g] * part[local:]
        square = jnp.mean(attended * attended, axis=-1, keepdims=True)
        made[i, g] = (attended * lax.rsqrt(square + 1e-06) * gain).astype(BF16)

    def finish(i):
        @pl.when(me != i)
        def _():
            give(i).start()

        @pl.when(me == i)
        def _():
            for g in range(mine):
                back[me * mine + g] = made[i, g]

    if n <= UNROLL:
        for i in range(n):
            arrive(i)
            for g in range(mine):
                attend(i, (i + 1) * local, g)
            finish(i)
    else:
        for j in range(n):
            arrive(j)

        def body(i, carry):
            for g in range(mine):
                attend(i, n * local, g)
            finish(i)
            return carry

        lax.fori_loop(0, n, body, 0)

    for p in peers:
        pltpu.make_async_remote_copy(
            src_ref=made.at[p],
            dst_ref=back.at[pl.ds(p * mine, mine)],
            send_sem=osend_sem.at[p],
            recv_sem=orecv_sem.at[p],
            device_id=there(p),
            device_id_type=pl.DeviceIdType.MESH,
        ).wait_recv()
    for p in peers:
        for t in range(3):
            push(t, p).wait_send()
        give(p).wait_send()


def pair_kernel(
    heads, local, qk, hw_ref, gain_hbm, q_hbm, k_hbm, v_hbm, back,
    rows_in, gq, gk, gv, lent, made, gain_ref, weight, in_sem, wsend_sem, wrecv_sem,
    send_sem, recv_sem, qsend_sem, qrecv_sem, osend_sem, orecv_sem,
):
    dim = q_hbm.shape[-1]
    moved = heads // 4
    me = lax.axis_index("sp")
    tokens = max(16, 256 // heads)
    chunk = tokens * heads
    across = lax.rem(me + CORES, 2 * CORES)
    beside = me + 1 - 2 * lax.rem(me, CORES)
    gathered = (gk, gv)

    loads = [
        pltpu.make_async_copy(src, rows_in.at[t], in_sem.at[t])
        for t, src in enumerate((k_hbm, v_hbm, q_hbm))
    ]
    loads.append(pltpu.make_async_copy(gain_hbm, gain_ref, in_sem.at[3]))
    for load in loads:
        load.start()
    barrier = pltpu.get_barrier_semaphore()
    others = [lax.rem(me + d, 2 * CORES) for d in range(1, 2 * CORES)]
    for p in others:
        pl.semaphore_signal(
            barrier, inc=1, device_id={"sp": p}, device_id_type=pl.DeviceIdType.MESH
        )
    mine = heads // (2 * CORES)
    for g in range(mine):
        weight[me * mine + g] = jnp.full((1, dim), hw_ref[g], F32)

    def tell(p, j):
        rows = weight.at[pl.ds(j * mine, mine)]
        return pltpu.make_async_remote_copy(
            src_ref=rows, dst_ref=rows,
            send_sem=wsend_sem.at[p], recv_sem=wrecv_sem.at[j],
            device_id={"sp": p}, device_id_type=pl.DeviceIdType.MESH,
        )

    order = order_matrix(chunk, heads, tokens, False)

    def relay(t):
        loads[t].wait()
        for c in range(local // tokens):
            rows = jnp.dot(
                order, rows_in[t, c * chunk:(c + 1) * chunk], preferred_element_type=F32
            ).astype(BF16)
            for h in range(heads):
                piece = rows[h * tokens:(h + 1) * tokens]
                if t == 2:
                    gq[h, c * tokens:(c + 1) * tokens] = piece
                else:
                    start = pl.multiple_of(me * local + c * tokens, tokens)
                    gathered[t][h, pl.ds(start, tokens)] = piece

    def block(t, h, j):
        start = j * local if isinstance(j, int) else pl.multiple_of(j * local, local)
        return gathered[t].at[h, pl.ds(start, local)]

    def move(t, h, j, p, kind):
        return pltpu.make_async_remote_copy(
            src_ref=block(t, h, j),
            dst_ref=block(t, h, j),
            send_sem=send_sem.at[kind, t, h, j],
            recv_sem=recv_sem.at[t, h, j],
            device_id={"sp": p},
            device_id_type=pl.DeviceIdType.MESH,
        )

    def lend(h, p):
        return pltpu.make_async_remote_copy(
            src_ref=gq.at[h], dst_ref=lent.at[h],
            send_sem=qsend_sem.at[h], recv_sem=qrecv_sem.at[h],
            device_id={"sp": p}, device_id_type=pl.DeviceIdType.MESH,
        )

    def give(h, p):
        return pltpu.make_async_remote_copy(
            src_ref=made.at[h], dst_ref=back.at[h],
            send_sem=osend_sem.at[h], recv_sem=orecv_sem.at[h],
            device_id={"sp": p}, device_id_type=pl.DeviceIdType.MESH,
        )

    relay(0)
    pl.semaphore_wait(barrier, 2 * CORES - 1)
    for p in others:
        tell(p, me).start()

    @pl.when(me < CORES)
    def _():
        move(0, moved, me, across, 0).start()

    @pl.when(me >= CORES)
    def _():
        move(0, 0, me, across, 0).start()

    relay(1)
    relay(2)
    loads[3].wait()
    gain = gain_ref[...]
    lower = lax.broadcasted_iota(jnp.int32, (local, dim), 1) < qk
    row = lax.rem(lax.broadcasted_iota(jnp.int32, (2 * local, local), 0), local)
    col = lax.broadcasted_iota(jnp.int32, (2 * local, local), 1)
    visible = col // SEGMENT <= row // SEGMENT

    def weigh(query, h, i):
        query = query * BF16(qk ** -0.5)
        zero = jnp.zeros_like(query)
        both = jnp.concatenate([jnp.where(lower, query, zero), jnp.where(lower, zero, query)], 0)
        across_dim = (((1,), (1,)), ((), ()))
        scores = lax.dot_general(
            both, gk[h, i * local:(i + 1) * local], across_dim, preferred_element_type=F32
        )
        scores = jnp.where(visible, scores, -jnp.inf)
        if i:
            past = lax.dot_general(
                both, gk[h, :i * local], across_dim, preferred_element_type=F32
            )
            scores = jnp.concatenate([past, scores], 1)
        raised = jnp.exp(scores - jnp.max(scores, axis=-1, keepdims=True))
        return raised.astype(BF16), jnp.sum(raised, axis=-1, keepdims=True)

    def mix(raised, total, h, i, late=None, wait=None):
        if late is None:
            part = jnp.dot(raised, gv[h, :(i + 1) * local], preferred_element_type=F32)
        else:
            part = 0.0
            for j in [j for j in range(i + 1) if j != late] + [late]:
                if j == late:
                    wait()
                at = slice(j * local, (j + 1) * local)
                part += jnp.dot(raised[:, at], gv[h, at], preferred_element_type=F32)
        part = part / total
        attended = part[:local] - weight[h] * part[local:]
        square = jnp.mean(attended * attended, axis=-1, keepdims=True)
        return (attended * lax.rsqrt(square + 1e-06) * gain).astype(BF16)

    def role(r):
        side, other = r + 1 - 2 * (r % CORES), (r + CORES) % (2 * CORES)
        sent = []

        def go(copy, begun=False):
            if not begun:
                copy.start()
            sent.append(copy)

        def hear():
            for p in range(2 * CORES):
                if p != r:
                    tell(p, p).wait_recv()

        def landed(t, h, j):
            move(t, h, j, side, 1).wait_recv()

        def pass_on(t, h, j):
            landed(t, h, j)
            go(move(t, h, j, side, 1))

        if r < CORES:
            for h in range(moved, heads):
                for t in range(2):
                    go(move(t, h, r, other, 0), begun=(h == moved and t == 0))
            for h in range(heads if r == 0 else moved):
                for t in range(2):
                    go(move(t, h, r, side, 1))
            hear()
            for h in range(heads):
                if r:
                    landed(0, h, 0)
                    landed(1, h, 0)
                back[h] = mix(*weigh(gq[h], h, r), h, r)
            for h in range(moved):
                if r == 0:
                    pass_on(0, h, other)
                    pass_on(1, h, other)
                    landed(0, h, 1)
                    landed(1, h, 1)
                else:
                    landed(0, h, other)
                    landed(0, h, other - 1)
                lend(h, other).wait_recv()
                weights = weigh(lent[h], h, other)
                if r:
                    landed(1, h, other)
                    landed(1, h, other - 1)
                made[h] = mix(*weights, h, other)
                go(give(h, other))
        else:
            for h in range(moved):
                for t in range(2):
                    go(move(t, h, r, other, 0), begun=(h == 0 and t == 0))
                go(lend(h, other))
            if r == CORES:
                for h in range(moved, heads):
                    for t in range(2):
                        go(move(t, h, r, side, 1))
            hear()
            far = side - CORES
            pass_on(0, moved, other)
            for h in range(moved, heads):
                pass_on(1, h, other)
                if h + 1 < heads:
                    pass_on(0, h + 1, other)
                landed(0, h, far)
                if r > CORES:
                    landed(0, h, side)
                weights = weigh(gq[h], h, r)
                if r > CORES:
                    landed(1, h, side)
                back[h] = mix(*weights, h, r, far, functools.partial(landed, 1, h, far))
            for h in range(moved):
                give(h, other).wait_recv()
        for copy in sent:
            copy.wait_send()

    for r in range(2 * CORES):
        pl.when(me == r)(functools.partial(role, r))
    for p in others:
        tell(p, me).wait_send()


def interleave(heads, local, back_ref, out_ref):
    tokens = max(16, 256 // heads)
    chunk = tokens * heads
    order = order_matrix(chunk, heads, tokens, True)
    for c in range(local // tokens):
        piece = jnp.concatenate(
            [back_ref[h, c * tokens:(c + 1) * tokens] for h in range(heads)], 0
        )
        out_ref[c * chunk:(c + 1) * chunk] = jnp.dot(
            order, piece, preferred_element_type=F32
        ).astype(BF16)


def on_device(n, query_rows, key_rows, value_rows, map_weight, head_gain):
    _, local, heads, dim = query_rows.shape
    mine = heads // n
    flat = (local * heads, dim)
    whole = n * local
    paired = n == 2 * CORES and heads % 4 == 0
    if paired:
        moved = heads // 4
        body = functools.partial(pair_kernel, heads, local, dim // 2)
        scratch = [
            pltpu.VMEM((heads, local, dim), BF16),
            pltpu.VMEM((heads, whole, dim), BF16),
            pltpu.VMEM((heads, whole, dim), BF16),
            pltpu.VMEM((moved, local, dim), BF16),
            pltpu.VMEM((moved, local, dim), BF16),
            pltpu.VMEM((1, dim), F32),
            pltpu.VMEM((heads, 1, dim), F32),
            pltpu.SemaphoreType.DMA((4,)),
            pltpu.SemaphoreType.DMA((n,)),
            pltpu.SemaphoreType.DMA((n,)),
            pltpu.SemaphoreType.DMA((2, 2, heads, n)),
            pltpu.SemaphoreType.DMA((2, heads, n)),
        ] + [pltpu.SemaphoreType.DMA((moved,))] * 4
    else:
        body = functools.partial(kernel, n, heads, local, dim // 2)
        scratch = [
            pltpu.VMEM((3, heads, local, dim), BF16),
            pltpu.VMEM((mine, whole, dim), BF16),
            pltpu.VMEM((mine, whole, dim), BF16),
            pltpu.VMEM((mine, whole, dim), BF16),
            pltpu.VMEM((n, mine, local, dim), BF16),
            pltpu.VMEM((1, dim), F32),
            pltpu.SemaphoreType.DMA((4,)),
            pltpu.SemaphoreType.DMA((3, n)),
            pltpu.SemaphoreType.DMA((3, n)),
            pltpu.SemaphoreType.DMA((n,)),
            pltpu.SemaphoreType.DMA((n,)),
        ]
    out = pl.pallas_call(
        body,
        out_shape=pltpu.VMEM((heads, local, dim), BF16),
        in_specs=[pl.BlockSpec(memory_space=pltpu.SMEM)]
        + [pl.BlockSpec(memory_space=pltpu.HBM)] * 4,
        out_specs=pl.BlockSpec(memory_space=pltpu.VMEM),
        scratch_shapes=[pltpu.VMEM((3,) + flat, BF16)] + scratch,
        compiler_params=pltpu.CompilerParams(collective_id=0, has_side_effects=True),
    )(
        map_weight,
        head_gain.reshape(1, dim),
        query_rows.reshape(flat),
        key_rows.reshape(flat),
        value_rows.reshape(flat),
    )
    rows = pl.pallas_call(
        functools.partial(interleave, heads, local),
        out_shape=jax.ShapeDtypeStruct(flat, BF16),
        in_specs=[pl.BlockSpec(memory_space=pltpu.VMEM)],
        out_specs=pl.BlockSpec(memory_space=pltpu.VMEM),
        compiler_params=pltpu.CompilerParams(vmem_limit_bytes=KERNEL_BYTES),
    )(out)
    return rows.reshape(query_rows.shape)


def solution(mesh):
    rows = P("dp", "sp", None, None)
    return jax.shard_map(
        functools.partial(on_device, mesh.shape["sp"]),
        mesh=mesh,
        in_specs=(rows, rows, rows, P("sp"), P()),
        out_specs=rows,
        check_vma=False,
    )
```
